32 devices in a mesh: ep: 16 (over z, y, x), tp: 2 (over core).
Axes of the slice: x: 2, y: 2, z: 4, core: 2. Of those that a mesh axis runs over, the one named last changes fastest.
Arguments:
- tokens: bfloat16 [768, 2048], P('ep', 'tp'), may hold values from -12 to 12
- conv_state: bfloat16 [768, 3, 1024], P('ep', None, 'tp'), may hold values from -6 to 6
- hidden_state: float32 [768, 1024], P('ep', 'tp'), may hold values from -6 to 6
- mixer_gain: float32 [2048], replicated, may hold values from 0.1 to 1.9
- branch_weight: bfloat16 [2048, 1024], P(None, 'tp'), may hold values from -0.125 to 0.125
- gelu_weight: bfloat16 [2048, 1024], P(None, 'tp'), may hold values from -0.125 to 0.125
- conv_kernel: float32 [4, 1024], P(None, 'tp'), may hold values from -3 to 3
- recur_blocks: bfloat16 [16, 64, 64], P('tp'), may hold values from -0.75 to 0.75
- input_blocks: bfloat16 [16, 64, 64], P('tp'), may hold values from -0.75 to 0.75
- decay_rate: float32 [1024], P('tp'), may hold values from 0.002 to 0.1
- output_weight: bfloat16 [1024, 2048], P(None, 'tp'), may hold values from -0.1875 to 0.1875
- expert_gain: float32 [2048], replicated, may hold values from 0.1 to 1.9
- expert_ids: int32 [768, 2], P('ep'), may hold values from 0 to 15, as said below
- group_prob: float32 [768], P('ep'), may hold values from 0.25 to 1
- expert_logit: float32 [768, 2], P('ep'), may hold values from -4 to 4
- expert_gate: bfloat16 [16, 2048, 512], P('ep', None, 'tp'), may hold values from -0.125 to 0.125
- expert_up: bfloat16 [16, 2048, 512], P('ep', None, 'tp'), may hold values from -0.125 to 0.125
- expert_down: bfloat16 [16, 512, 2048], P('ep', 'tp'), may hold values from -0.25 to 0.25
Outputs:
- layer_out: bfloat16 [768, 2048], P('ep', 'tp')
- new_hidden: float32 [768, 1024], P('ep', 'tp')
The draws below stay inside these ranges and needn't reach their ends.
Inputs may be any that keep to these rules, and one draw needn't show every extreme that they name: `expert_ids`: the two experts of a row are different and lie in one group of 4 consecutive experts. Within the rows of one index of ep no expert is named more than 6 times, and one expert is named exactly 6 times by the rows of every index of ep.
All inputs are finite; a program needn't handle non-finite values.
Results may differ from the reference program's by a relative error of at most 0.012.
Values may be sent and summed in bfloat16 or wider, within the bound.
A program may use at most 64 MiB of HBM per device.

```python
import math
import jax
import jax.numpy as jnp
from jax import lax

D = 2048
LRU = 1024
BLOCK = 64
CONV = 4
FF = 512
GROUPS = 4
TOP = 2
SEQ_DEV = 48
EXPERTS = 16
EXPERTS_GROUP = 4
CAP = 6
TOKENS = 768
N_EP = 16
N_TP = 2


def draw_tokens(key, part):
    first_key = jax.random.fold_in(key, 0)
    columns = jnp.arange(D, dtype=jnp.float32) / (D - 1)
    column_scale = jnp.exp(jnp.log(0.5) + jnp.log(4.0) * columns)
    values = jnp.clip(jax.random.normal(first_key, (TOKENS, D), jnp.float32), -3.0, 3.0)
    return (values * column_scale[None, :]).astype(jnp.bfloat16)


def draw_expert_ids(key, part):
    devices = TOKENS // SEQ_DEV
    hot_key, round_key, score_key, shuffle_key = jax.random.split(jax.random.fold_in(key, 7), 4)
    hot_expert = jax.random.randint(hot_key, (), 0, EXPERTS)
    round_keys = jax.random.split(round_key, devices * GROUPS * CAP)
    orders = jax.vmap(lambda single: jax.random.permutation(single, EXPERTS_GROUP))(round_keys)
    orders = orders.reshape(devices, GROUPS, CAP, EXPERTS_GROUP).astype(jnp.int32)
    group_base = (jnp.arange(GROUPS, dtype=jnp.int32) * EXPERTS_GROUP)[None, :, None, None]
    members = (orders + group_base).reshape(devices, GROUPS * CAP * (EXPERTS_GROUP // 2), 2)
    candidates = members.shape[1]
    is_hot = jnp.any(members == hot_expert, axis=2).astype(jnp.int32)
    scores = jax.random.randint(score_key, (devices, candidates), 0, 1 << 16)
    keyed = scores * candidates + jnp.arange(candidates, dtype=jnp.int32)[None, :] + (1 - is_hot) * (1 << 29)
    order = jnp.argsort(keyed, axis=1)[:, :SEQ_DEV]
    chosen = jnp.take_along_axis(members, order[:, :, None], axis=1)
    shuffles = jax.vmap(lambda single: jax.random.permutation(single, SEQ_DEV))(jax.random.split(shuffle_key, devices))
    shuffled = jnp.take_along_axis(chosen, shuffles[:, :, None].astype(jnp.int32), axis=1)
    return shuffled.reshape(TOKENS, 2).astype(jnp.int32)


def levels(key, dims, cuts, low, largest):
    def one(axis_at, shards_of):
        heights = jax.random.uniform(jax.random.fold_in(jax.random.fold_in(key, 6), axis_at), (shards_of,), jnp.float32, low / len(cuts), largest / len(cuts))
        return jnp.repeat(jnp.exp(heights), dims[axis_at] // shards_of).reshape((-1,) + (1,) * (len(dims) - axis_at - 1))

    factor_of = one(*cuts[0])
    for cut in cuts[1:]:
        factor_of = factor_of * one(*cut)
    return factor_of


def centred(own_key, extent, scale, limit, pieces=(), kind=jnp.bfloat16):
    loudness = levels(own_key, extent, pieces, -0.22, 0.18) if pieces else 1.0
    entries = jax.random.normal(own_key, extent, jnp.float32) * scale * loudness
    return jnp.minimum(jnp.maximum(entries, -limit), limit).astype(kind)


def setup_inputs(seed: int = 0) -> dict:
    key_list = jax.random.split(jax.random.key(seed), 19)
    return {
        "tokens": draw_tokens(jax.random.fold_in(key_list[18], 71), 0),
        "conv_state": centred(key_list[1], (TOKENS, CONV - 1, LRU), 1.0, 6.0, ((0, 16), (2, 2))),
        "hidden_state": centred(key_list[2], (TOKENS, LRU), 1.0, 6.0, ((0, 16), (1, 2)), jnp.float32),
        "mixer_gain": jnp.clip(1.0 + 0.18 * jax.random.normal(key_list[3], (D,), jnp.float32), 0.1, 1.9),
        "branch_weight": centred(key_list[4], (D, LRU), D ** -0.5, 0.125, ((1, 2),)),
        "gelu_weight": centred(key_list[5], (D, LRU), D ** -0.5, 0.125, ((1, 2),)),
        "conv_kernel": centred(key_list[6], (CONV, LRU), CONV ** -0.5, 3.0, ((1, 2),), jnp.float32),
        "recur_blocks": centred(key_list[7], (LRU // BLOCK, BLOCK, BLOCK), BLOCK ** -0.5, 0.75, ((0, 2),)),
        "input_blocks": centred(key_list[8], (LRU // BLOCK, BLOCK, BLOCK), BLOCK ** -0.5, 0.75, ((0, 2),)),
        "decay_rate": jnp.clip(jnp.exp(math.log(0.1) - 3.912023 * jax.random.uniform(key_list[9], (LRU,), jnp.float32) ** levels(key_list[9], (LRU,), ((0, 2),), -0.2, 0.2)), 0.002, 0.1),
        "output_weight": centred(key_list[10], (LRU, D), LRU ** -0.5, 0.1875, ((1, 2),)),
        "expert_gain": jnp.clip(1.0 + 0.18 * jax.random.normal(key_list[11], (D,), jnp.float32), 0.1, 1.9),
        "expert_ids": draw_expert_ids(jax.random.fold_in(key_list[18], 71), 0),
        "group_prob": jnp.clip(0.25 + 0.75 * jax.random.uniform(key_list[13], (TOKENS,), jnp.float32) ** levels(key_list[13], (TOKENS,), ((0, 16),), -0.2, 0.2), 0.25, 1.0),
        "expert_logit": centred(key_list[14], (TOKENS, TOP), 1.0, 4.0, ((0, 16),), jnp.float32),
        "expert_gate": centred(key_list[15], (EXPERTS, D, FF), D ** -0.5, 0.125, ((0, 16), (2, 2))),
        "expert_up": centred(key_list[16], (EXPERTS, D, FF), D ** -0.5, 0.125, ((0, 16), (2, 2))),
        "expert_down": centred(key_list[17], (EXPERTS, FF, D), FF ** -0.5, 0.25, ((0, 16), (1, 2))),
    }


EPSILON = 1e-06
RATE_SCALE = 8.0

def normalize(values, gain_row):
    squares = lax.optimization_barrier(jnp.mean(values * values, axis=-1, keepdims=True))
    return values * lax.rsqrt(squares + EPSILON) * gain_row

def reference(tokens, conv_state, hidden_state, mixer_gain, branch_weight, gelu_weight, conv_kernel, recur_blocks, input_blocks, decay_rate, output_weight, expert_gain, expert_ids, group_prob, expert_logit, expert_gate, expert_up, expert_down):
    normed = normalize(tokens.astype(jnp.float32), mixer_gain).astype(jnp.bfloat16)
    branch = jnp.dot(normed, branch_weight, preferred_element_type=jnp.float32).astype(jnp.bfloat16)
    gelu_input = jnp.dot(normed, gelu_weight, preferred_element_type=jnp.float32).astype(jnp.bfloat16)
    window = jnp.concatenate([conv_state, branch[:, None, :]], axis=1).astype(jnp.float32)
    convolved = lax.optimization_barrier(jnp.sum(window * conv_kernel[None], axis=1)).astype(jnp.bfloat16)
    grouped = convolved.reshape(TOKENS, LRU // BLOCK, BLOCK).astype(jnp.float32)
    recur_pre = jnp.einsum('tnc,ncd->tnd', grouped, recur_blocks.astype(jnp.float32)).reshape(TOKENS, LRU)
    input_pre = jnp.einsum('tnc,ncd->tnd', grouped, input_blocks.astype(jnp.float32)).reshape(TOKENS, LRU)
    recur_gate = jax.nn.sigmoid(recur_pre)
    input_gate = jax.nn.sigmoid(input_pre)
    log_decay = -RATE_SCALE * recur_gate * decay_rate
    new_hidden = jnp.exp(log_decay) * hidden_state + jnp.sqrt(-jnp.expm1(2.0 * log_decay)) * (input_gate * convolved.astype(jnp.float32))
    mixed_rows = (new_hidden * jax.nn.gelu(gelu_input.astype(jnp.float32), approximate=True)).astype(jnp.bfloat16)
    residual = (tokens.astype(jnp.float32) + jnp.dot(mixed_rows, output_weight, preferred_element_type=jnp.float32)).astype(jnp.bfloat16)
    moe_input = normalize(residual.astype(jnp.float32), expert_gain).astype(jnp.bfloat16)
    sources = jnp.arange(TOKENS * TOP, dtype=jnp.int32) // (SEQ_DEV * TOP)
    block_ids = expert_ids.reshape(N_EP, SEQ_DEV * TOP)
    onehot_ids = (block_ids[:, :, None] == jnp.arange(EXPERTS, dtype=jnp.int32)[None, None, :]).astype(jnp.int32)
    earlier = jnp.cumsum(onehot_ids, axis=1) - onehot_ids
    ranking = lax.optimization_barrier(jnp.sum(earlier * onehot_ids, axis=2)).reshape(-1)
    flat_ids = expert_ids.reshape(-1)
    slot_index = flat_ids * (N_EP * CAP) + sources * CAP + ranking
    token_index = jnp.arange(TOKENS * TOP, dtype=jnp.int32) // TOP
    table = jnp.full((EXPERTS * N_EP * CAP,), TOKENS, jnp.int32).at[slot_index].set(token_index).reshape(EXPERTS, N_EP * CAP)
    padded = jnp.concatenate([moe_input, jnp.zeros((1, D), jnp.bfloat16)], axis=0)

    def one_expert(operands):
        indices, gate_matrix, upper_matrix, down_matrix = operands
        gathered = jnp.take(padded, indices, axis=0)
        gate_part = jnp.dot(gathered, gate_matrix, preferred_element_type=jnp.float32)
        upper_part = jnp.dot(gathered, upper_matrix, preferred_element_type=jnp.float32)
        hidden_units = (jax.nn.silu(gate_part) * upper_part).astype(jnp.bfloat16)
        split_width = FF // N_TP
        total = jnp.zeros((N_EP * CAP, D), jnp.float32)
        for member in range(N_TP):
            piece = jnp.dot(hidden_units[:, member * split_width:(member + 1) * split_width], down_matrix[member * split_width:(member + 1) * split_width], preferred_element_type=jnp.float32)
            total = total + piece.astype(jnp.bfloat16).astype(jnp.float32)
        return total.astype(jnp.bfloat16)
    outcome = lax.map(one_expert, (table, expert_gate, expert_up, expert_down))
    picked = jnp.take(outcome.reshape(EXPERTS * N_EP * CAP, D), slot_index, axis=0).reshape(TOKENS, TOP, D)
    logit_exp = jnp.exp(expert_logit)
    weights = group_prob[:, None] * logit_exp / lax.optimization_barrier(jnp.sum(logit_exp, axis=1, keepdims=True))
    layer_out = (residual.astype(jnp.float32) + lax.optimization_barrier(jnp.sum(weights[:, :, None] * picked.astype(jnp.float32), axis=1))).astype(jnp.bfloat16)
    return (layer_out, new_hidden)
```

```python
import functools

import jax
import jax.numpy as jnp
from jax import lax
from jax.experimental import pallas as pl
from jax.experimental.pallas import tpu as pltpu
from jax.sharding import PartitionSpec as P

EPSILON = 1e-06
RATE_SCALE = 8.0
MESH = pl.DeviceIdType.MESH
F32 = jnp.float32
BF16 = jnp.bfloat16


def iota(shape, dim):
    return lax.broadcasted_iota(jnp.int32, shape, dim)


def dot(a, b):
    return jnp.dot(a, b, preferred_element_type=F32)


def minus_expm1(z):
    series = 1.0
    for term in (7.0, 6.0, 5.0, 4.0, 3.0, 2.0):
        series = 1.0 + z * (1.0 / term) * series
    return jnp.where(z > -0.35, -z * series, 1.0 - jnp.exp(z))


def kernel(
    n_ep,
    cap,
    tokens,
    conv_state,
    hidden_state,
    mixer_gain,
    branch_weight,
    gelu_weight,
    conv_kernel,
    recur_blocks,
    input_blocks,
    decay_rate,
    output_weight,
    expert_gain,
    expert_ids,
    group_prob,
    expert_logit,
    expert_gate,
    expert_up,
    expert_down,
    layer_out,
    new_hidden_ref,
    w_branch,
    w_gelu,
    w_out,
    w_gate,
    w_up,
    w_down,
    tok,
    mixed,
    squares,
    outgoing,
    recv,
    stage,
    hid,
    ret,
    back,
    back_stage,
    load_sem,
    pair_send,
    pair_recv,
    far_send,
    far_recv,
):
    ep = lax.axis_index("ep")
    tp = lax.axis_index("tp")
    other = 1 - tp
    seq, half = tokens.shape
    chans = hidden_state.shape[1]
    pad = stage.shape[2]
    slots = n_ep * pad

    mine = pl.ds(pl.multiple_of(tp * half, half), half)
    theirs = pl.ds(pl.multiple_of(other * half, half), half)

    loads = [
        pltpu.make_async_copy(branch_weight.at[mine], w_branch.at[tp], load_sem.at[0]),
        pltpu.make_async_copy(gelu_weight.at[mine], w_gelu.at[tp], load_sem.at[1]),
        pltpu.make_async_copy(branch_weight.at[theirs], w_branch.at[other], load_sem.at[2]),
        pltpu.make_async_copy(gelu_weight.at[theirs], w_gelu.at[other], load_sem.at[3]),
        pltpu.make_async_copy(output_weight, w_out, load_sem.at[4]),
        pltpu.make_async_copy(expert_gate.at[0], w_gate, load_sem.at[5]),
        pltpu.make_async_copy(expert_up.at[0], w_up, load_sem.at[6]),
        pltpu.make_async_copy(expert_down.at[0, :, mine], w_down.at[tp], load_sem.at[7]),
    ]
    for load in loads:
        load.start()

    barrier = pltpu.get_barrier_semaphore()
    pl.semaphore_signal(barrier, inc=1, device_id=(ep, other), device_id_type=MESH)

    def greet(step, carry):
        pl.semaphore_signal(
            barrier, inc=1, device_id=(lax.rem(ep + step, n_ep), tp), device_id_type=MESH
        )
        return carry

    lax.fori_loop(1, n_ep, greet, 0)

    def to_pair(src, dst, index):
        return pltpu.make_async_remote_copy(
            src_ref=src,
            dst_ref=dst,
            send_sem=pair_send.at[index],
            recv_sem=pair_recv.at[index],
            device_id=(ep, other),
            device_id_type=MESH,
        )

    stage[...] = jnp.zeros_like(stage)
    back_stage[...] = jnp.zeros_like(back_stage)
    eye = iota((seq, seq), 0) == iota((seq, seq), 1)
    ids = expert_ids[...]
    first, second = ids[:, 0:1], ids[:, 1:2]
    lane_e = iota((seq, n_ep), 1)
    is_first, is_second = lane_e == first, lane_e == second
    named = jnp.where(is_first | is_second, 1.0, 0.0).astype(BF16)
    before = jnp.where(iota((seq, seq), 1) < iota((seq, seq), 0), 1.0, 0.0).astype(BF16)
    earlier = dot(before, named)

    def slot_of(chosen, hits):
        rank = jnp.sum(jnp.where(hits, earlier, 0.0), axis=1, keepdims=True)
        return chosen.astype(F32) * float(pad) + rank

    slot_a, slot_b = slot_of(first, is_first), slot_of(second, is_second)

    def as_row(column):
        return jnp.sum(jnp.where(eye, column, 0.0), axis=0, keepdims=True)

    lane_s = iota((seq, slots), 1).astype(F32)
    pick_a = jnp.where(lane_s == slot_a, 1.0, 0.0).astype(BF16)
    pick_b = jnp.where(lane_s == slot_b, 1.0, 0.0).astype(BF16)
    row_s = iota((slots, seq), 0).astype(F32)
    placed = (row_s == as_row(slot_a)) | (row_s == as_row(slot_b))
    placing = jnp.where(placed, 1.0, 0.0).astype(BF16)
    prob = jnp.sum(jnp.where(eye, group_prob[...], 0.0), axis=1, keepdims=True)
    logit_exp = jnp.exp(expert_logit[...])
    weights = prob * logit_exp / jnp.sum(logit_exp, axis=1, keepdims=True)

    taps = conv_kernel[...]
    stored = jnp.sum(conv_state[...].astype(F32) * taps[None, :3], axis=1)

    blocks, block = recur_blocks.shape[0], recur_blocks.shape[1]
    wide = 2 * block
    twice = jnp.where(
        lax.rem(iota((block, wide), 1), block) == iota((block, wide), 0), 1.0, 0.0
    ).astype(BF16)
    on_diagonal = (iota((wide, wide), 0) < block) == (iota((wide, wide), 1) < block)

    def pair_map(ref, index):
        rows = jnp.concatenate([ref[2 * index], ref[2 * index + 1]], axis=0)
        return jnp.where(on_diagonal, dot(rows, twice), 0.0).astype(BF16)

    recur_maps = [pair_map(recur_blocks, i) for i in range(blocks // 2)]
    input_maps = [pair_map(input_blocks, i) for i in range(blocks // 2)]

    own = tokens[...].astype(F32)
    own_scaled = (own * mixer_gain[:, mine]).astype(BF16)
    own_square = jnp.sum(own * own, axis=1, keepdims=True)
    loads[0].wait()
    branch = dot(own_scaled, w_branch[tp])
    loads[1].wait()
    gelu_input = dot(own_scaled, w_gelu[tp])

    pl.semaphore_wait(barrier, n_ep)
    send_tokens = to_pair(tokens, tok, 0)
    send_tokens.start()
    send_down = to_pair(expert_down.at[0, :, theirs], w_down.at[tp], 1)
    send_down.start()

    send_tokens.wait_recv()
    peer = tok[...].astype(F32)
    peer_scaled = (peer * mixer_gain[:, theirs]).astype(BF16)
    total_square = own_square + jnp.sum(peer * peer, axis=1, keepdims=True)
    scale = lax.rsqrt(total_square / (2 * half) + EPSILON)
    loads[2].wait()
    branch = ((branch + dot(peer_scaled, w_branch[other])) * scale).astype(BF16)
    loads[3].wait()
    gelu_input = ((gelu_input + dot(peer_scaled, w_gelu[other])) * scale).astype(BF16)

    convolved = (stored + branch.astype(F32) * taps[3:4]).astype(BF16)
    pieces = [convolved[:, wide * i : wide * (i + 1)] for i in range(blocks // 2)]
    recur_pre = jnp.concatenate([dot(x, m) for x, m in zip(pieces, recur_maps)], axis=1)
    input_pre = jnp.concatenate([dot(x, m) for x, m in zip(pieces, input_maps)], axis=1)
    recur_gate = jax.nn.sigmoid(recur_pre)
    input_gate = jax.nn.sigmoid(input_pre)
    log_decay = -RATE_SCALE * recur_gate * decay_rate[...]
    new_hidden = jnp.exp(log_decay) * hidden_state[...] + jnp.sqrt(
        minus_expm1(2.0 * log_decay)
    ) * (input_gate * convolved.astype(F32))
    mixed[tp] = (new_hidden * jax.nn.gelu(gelu_input.astype(F32), approximate=True)).astype(BF16)
    send_mixed = to_pair(mixed.at[tp], mixed.at[tp], 2)
    send_mixed.start()
    new_hidden_ref[...] = new_hidden
    loads[4].wait()
    my_rows = pl.ds(pl.multiple_of(tp * chans, chans), chans)
    their_rows = pl.ds(pl.multiple_of(other * chans, chans), chans)
    residual = own + dot(mixed[tp], w_out[my_rows])
    send_mixed.wait_recv()
    residual = (residual + dot(mixed[other], w_out[their_rows])).astype(BF16)

    values = residual.astype(F32)
    mine_square = jnp.sum(values * values, axis=1, keepdims=True)
    squares[tp] = jnp.broadcast_to(mine_square, squares.shape[1:])
    send_squares = to_pair(squares.at[tp], squares.at[tp], 3)
    send_squares.start()
    chosen = dot(placing, residual) * expert_gain[:, mine]
    send_squares.wait_recv()
    both = mine_square + squares[other][:, 0:1]
    scaling = as_row(lax.rsqrt(both / (2 * half) + EPSILON))
    slot_scale = jnp.sum(jnp.where(placed, scaling, 0.0), axis=1, keepdims=True)
    chosen = (chosen * slot_scale).reshape(n_ep, pad, half)
    outgoing[...] = chosen[:, :cap].astype(BF16)

    def far(src, dst, to, index):
        return pltpu.make_async_remote_copy(
            src_ref=src,
            dst_ref=dst,
            send_sem=far_send.at[index],
            recv_sem=far_recv.at[index],
            device_id=(to, tp),
            device_id_type=MESH,
        )

    def dispatch(step, carry):
        to = lax.rem(ep + step, n_ep)
        far(outgoing.at[to], recv.at[tp, ep], to, 0).start()
        return carry

    lax.fori_loop(1, n_ep, dispatch, 0)
    recv[tp, ep] = outgoing[ep]
    some = pl.ds(0, n_ep - 1)
    all_dispatched = far(outgoing.at[some], recv.at[tp, some], ep, 0)
    all_dispatched.wait_recv()
    forward = to_pair(recv.at[tp], recv.at[tp], 4)
    forward.start()
    for load in loads[5:]:
        load.wait()
    stage[0, :, :cap] = recv[tp].astype(F32)
    own_rows = stage[0].reshape(slots, half).astype(BF16)
    gate_part = dot(own_rows, w_gate[mine])
    up_part = dot(own_rows, w_up[mine])
    forward.wait_recv()
    stage[1, :, :cap] = recv[other].astype(F32)
    peer_rows = stage[1].reshape(slots, half).astype(BF16)
    gate_part = gate_part + dot(peer_rows, w_gate[theirs])
    up_part = up_part + dot(peer_rows, w_up[theirs])
    hid[tp] = (jax.nn.silu(gate_part) * up_part).astype(BF16)
    send_hid = to_pair(hid.at[tp], hid.at[tp], 5)
    send_hid.start()
    result = dot(hid[tp], w_down[tp])
    send_down.wait_recv()
    send_hid.wait_recv()
    result = result + dot(hid[other], w_down[other])
    ret[...] = result.reshape(n_ep, pad, half)[:, :cap].astype(BF16)

    def give_back(step, carry):
        to = lax.rem(ep + step, n_ep)
        far(ret.at[to], back.at[ep], to, 1).start()
        return carry

    lax.fori_loop(1, n_ep, give_back, 0)
    back[ep] = ret[ep]
    all_returned = far(ret.at[some], back.at[some], ep, 1)
    all_returned.wait_recv()
    back_stage[:, :cap] = back[...].astype(F32)
    rows = back_stage[...].reshape(slots, half).astype(BF16)
    total = weights[:, 0:1] * dot(pick_a, rows) + weights[:, 1:2] * dot(pick_b, rows)
    layer_out[...] = (values + total).astype(BF16)

    for copy in (send_tokens, send_down, send_mixed, send_squares, forward, send_hid):
        copy.wait_send()
    all_dispatched.wait_send()
    all_returned.wait_send()


def local(n_ep, *args):
    names = list(args)
    tokens, conv_state, hidden_state = names[:3]
    seq, half = tokens.shape
    chans = hidden_state.shape[1]
    hidden_units = names[15].shape[2]
    cap = 2 * max(1, seq // n_ep)
    pad = -(-cap // 8) * 8
    for at in (3, 9, 11, 13):
        names[at] = names[at].reshape(1, -1)
    vmem = pl.BlockSpec(memory_space=pltpu.VMEM)
    hbm = pl.BlockSpec(memory_space=pl.ANY)
    specs = [vmem] * len(names)
    for at in (4, 5, 10, 15, 16, 17):
        specs[at] = hbm
    return pl.pallas_call(
        functools.partial(kernel, n_ep, cap),
        out_shape=(
            jax.ShapeDtypeStruct((seq, half), BF16),
            jax.ShapeDtypeStruct((seq, chans), F32),
        ),
        in_specs=specs,
        out_specs=(vmem, vmem),
        scratch_shapes=[
            pltpu.VMEM((2, half, chans), BF16),
            pltpu.VMEM((2, half, chans), BF16),
            pltpu.VMEM((2 * chans, half), BF16),
            pltpu.VMEM((2 * half, hidden_units), BF16),
            pltpu.VMEM((2 * half, hidden_units), BF16),
            pltpu.VMEM((2, hidden_units, half), BF16),
            pltpu.VMEM((seq, half), BF16),
            pltpu.VMEM((2, seq, chans), BF16),
            pltpu.VMEM((2, seq, 128), F32),
            pltpu.VMEM((n_ep, cap, half), BF16),
            pltpu.VMEM((2, n_ep, cap, half), BF16),
            pltpu.VMEM((2, n_ep, pad, half), F32),
            pltpu.VMEM((2, n_ep * pad, hidden_units), BF16),
            pltpu.VMEM((n_ep, cap, half), BF16),
            pltpu.VMEM((n_ep, cap, half), BF16),
            pltpu.VMEM((n_ep, pad, half), F32),
            pltpu.SemaphoreType.DMA((8,)),
            pltpu.SemaphoreType.DMA((6,)),
            pltpu.SemaphoreType.DMA((6,)),
            pltpu.SemaphoreType.DMA((2,)),
            pltpu.SemaphoreType.DMA((2,)),
        ],
        compiler_params=pltpu.CompilerParams(
            collective_id=0, has_side_effects=True, vmem_limit_bytes=60 * 1024 * 1024
        ),
    )(*names)


def solution(mesh):
    return jax.shard_map(
        functools.partial(local, mesh.shape["ep"]),
        mesh=mesh,
        in_specs=(
            P("ep", "tp"),
            P("ep", None, "tp"),
            P("ep", "tp"),
            P(),
            P(None, "tp"),
            P(None, "tp"),
            P(None, "tp"),
            P("tp", None, None),
            P("tp", None, None),
            P("tp"),
            P(None, "tp"),
            P(),
            P("ep", None),
            P("ep"),
            P("ep", None),
            P("ep", None, "tp"),
            P("ep", None, "tp"),
            P("ep", "tp", None),
        ),
        out_specs=(P("ep", "tp"), P("ep", "tp")),
        check_vma=False,
    )
```

```python
import functools

import jax
import jax.numpy as jnp
from jax import lax
from jax.experimental import pallas as pl
from jax.experimental.pallas import tpu as pltpu
from jax.sharding import PartitionSpec as P

EPSILON = 1e-06
RATE_SCALE = 8.0
VMEM_BYTES = 67_043_328
MESH = pl.DeviceIdType.MESH
F32 = jnp.float32
BF16 = jnp.bfloat16


def iota(shape, dim):
    return lax.broadcasted_iota(jnp.int32, shape, dim)


def dot(a, b):
    return jnp.dot(a, b, preferred_element_type=F32)


def minus_expm1(z):
    series = 1.0
    for term in (7.0, 6.0, 5.0, 4.0, 3.0, 2.0):
        series = 1.0 + z * (1.0 / term) * series
    return jnp.where(z > -0.35, -z * series, 1.0 - jnp.exp(z))


def kernel(
    n_ep,
    cap,
    tokens,
    conv_state,
    hidden_state,
    mixer_gain,
    branch_weight,
    gelu_weight,
    conv_kernel,
    recur_blocks,
    input_blocks,
    decay_rate,
    output_weight,
    expert_gain,
    expert_ids,
    group_prob,
    expert_logit,
    expert_gate,
    expert_up,
    expert_down,
    layer_out,
    new_hidden_ref,
    w_branch,
    w_gelu,
    w_out,
    w_gate,
    w_up,
    w_down,
    tok,
    mixed,
    squares,
    outgoing,
    recv,
    stage,
    hid,
    ret,
    back,
    back_stage,
    load_sem,
    pair_send,
    pair_recv,
    far_send,
    far_recv,
):
    ep = lax.axis_index("ep")
    tp = lax.axis_index("tp")
    other = 1 - tp
    seq, half = tokens.shape
    chans = hidden_state.shape[1]
    pad = stage.shape[2]
    slots = n_ep * pad

    mine = pl.ds(pl.multiple_of(tp * half, half), half)
    theirs = pl.ds(pl.multiple_of(other * half, half), half)

    loads = [
        pltpu.make_async_copy(branch_weight.at[mine], w_branch.at[tp], load_sem.at[0]),
        pltpu.make_async_copy(gelu_weight.at[mine], w_gelu.at[tp], load_sem.at[1]),
        pltpu.make_async_copy(branch_weight.at[theirs], w_branch.at[other], load_sem.at[2]),
        pltpu.make_async_copy(gelu_weight.at[theirs], w_gelu.at[other], load_sem.at[3]),
        pltpu.make_async_copy(output_weight, w_out, load_sem.at[4]),
        pltpu.make_async_copy(expert_gate.at[0], w_gate, load_sem.at[5]),
        pltpu.make_async_copy(expert_up.at[0], w_up, load_sem.at[6]),
        pltpu.make_async_copy(expert_down.at[0, :, mine], w_down.at[tp], load_sem.at[7]),
    ]
    for load in loads:
        load.start()

    barrier = pltpu.get_barrier_semaphore()
    pl.semaphore_signal(barrier, inc=1, device_id=(ep, other), device_id_type=MESH)

    def greet(step, carry):
        pl.semaphore_signal(
            barrier, inc=1, device_id=(lax.rem(ep + step, n_ep), tp), device_id_type=MESH
        )
        return carry

    lax.fori_loop(1, n_ep, greet, 0)

    def to_pair(src, dst, index):
        return pltpu.make_async_remote_copy(
            src_ref=src,
            dst_ref=dst,
            send_sem=pair_send.at[index],
            recv_sem=pair_recv.at[index],
            device_id=(ep, other),
            device_id_type=MESH,
        )

    stage[...] = jnp.zeros_like(stage)
    back_stage[...] = jnp.zeros_like(back_stage)
    eye = iota((seq, seq), 0) == iota((seq, seq), 1)

    def as_row(column):
        return jnp.sum(jnp.where(eye, column, 0.0), axis=0, keepdims=True)

    def as_column(row):
        return jnp.sum(jnp.where(eye, row, 0.0), axis=1, keepdims=True)

    ids = expert_ids[...].astype(F32)
    first, second = as_column(ids[0:1]), as_column(ids[1:2])
    lane_e = iota((seq, n_ep), 1).astype(F32)
    is_first, is_second = lane_e == first, lane_e == second
    named = jnp.where(is_first | is_second, 1.0, 0.0).astype(BF16)
    before = jnp.where(iota((seq, seq), 1) < iota((seq, seq), 0), 1.0, 0.0).astype(BF16)
    earlier = dot(before, named)

    def slot_of(chosen, hits):
        rank = jnp.sum(jnp.where(hits, earlier, 0.0), axis=1, keepdims=True)
        return chosen * float(pad) + rank

    slot_a, slot_b = slot_of(first, is_first), slot_of(second, is_second)

    lane_s = iota((seq, slots), 1).astype(F32)
    pick_a = jnp.where(lane_s == slot_a, 1.0, 0.0).astype(BF16)
    pick_b = jnp.where(lane_s == slot_b, 1.0, 0.0).astype(BF16)
    row_s = iota((slots, seq), 0).astype(F32)
    placed = (row_s == as_row(slot_a)) | (row_s == as_row(slot_b))
    placing = jnp.where(placed, 1.0, 0.0).astype(BF16)
    logit_exp = jnp.exp(expert_logit[...])
    weights = group_prob[...] * logit_exp / jnp.sum(logit_exp, axis=0, keepdims=True)
    weight_a, weight_b = as_column(weights[0:1]), as_column(weights[1:2])

    taps = conv_kernel[...]
    stored = sum(conv_state[j].astype(F32) * taps[j : j + 1] for j in range(3))

    blocks, block = recur_blocks.shape[0], recur_blocks.shape[1]
    wide = 2 * block
    twice = jnp.where(
        lax.rem(iota((block, wide), 1), block) == iota((block, wide), 0), 1.0, 0.0
    ).astype(BF16)
    on_diagonal = (iota((wide, wide), 0) < block) == (iota((wide, wide), 1) < block)

    def pair_map(ref, index):
        rows = jnp.concatenate([ref[2 * index], ref[2 * index + 1]], axis=0)
        return jnp.where(on_diagonal, dot(rows, twice), 0.0).astype(BF16)

    recur_maps = [pair_map(recur_blocks, i) for i in range(blocks // 2)]
    input_maps = [pair_map(input_blocks, i) for i in range(blocks // 2)]

    own = tokens[...].astype(F32)
    own_scaled = (own * mixer_gain[:, mine]).astype(BF16)
    own_square = jnp.sum(own * own, axis=1, keepdims=True)
    loads[0].wait()
    branch = dot(own_scaled, w_branch[tp])
    loads[1].wait()
    gelu_input = dot(own_scaled, w_gelu[tp])

    pl.semaphore_wait(barrier, n_ep)
    send_tokens = to_pair(tokens, tok, 0)
    send_tokens.start()
    send_down = to_pair(expert_down.at[0, :, theirs], w_down.at[tp], 1)
    send_down.start()

    send_tokens.wait_recv()
    peer = tok[...].astype(F32)
    peer_scaled = (peer * mixer_gain[:, theirs]).astype(BF16)
    total_square = own_square + jnp.sum(peer * peer, axis=1, keepdims=True)
    scale = lax.rsqrt(total_square / (2 * half) + EPSILON)
    loads[2].wait()
    branch = ((branch + dot(peer_scaled, w_branch[other])) * scale).astype(BF16)
    loads[3].wait()
    gelu_input = ((gelu_input + dot(peer_scaled, w_gelu[other])) * scale).astype(BF16)

    convolved = (stored + branch.astype(F32) * taps[3:4]).astype(BF16)
    pieces = [convolved[:, wide * i : wide * (i + 1)] for i in range(blocks // 2)]
    recur_pre = jnp.concatenate([dot(x, m) for x, m in zip(pieces, recur_maps)], axis=1)
    input_pre = jnp.concatenate([dot(x, m) for x, m in zip(pieces, input_maps)], axis=1)
    recur_gate = jax.nn.sigmoid(recur_pre)
    input_gate = jax.nn.sigmoid(input_pre)
    log_decay = -RATE_SCALE * recur_gate * decay_rate[...]
    new_hidden = jnp.exp(log_decay) * hidden_state[...] + jnp.sqrt(
        minus_expm1(2.0 * log_decay)
    ) * (input_gate * convolved.astype(F32))
    mixed[tp] = (new_hidden * jax.nn.gelu(gelu_input.astype(F32), approximate=True)).astype(BF16)
    send_mixed = to_pair(mixed.at[tp], mixed.at[tp], 2)
    send_mixed.start()
    new_hidden_ref[...] = new_hidden
    loads[4].wait()
    my_rows = pl.ds(pl.multiple_of(tp * chans, chans), chans)
    their_rows = pl.ds(pl.multiple_of(other * chans, chans), chans)
    residual = own + dot(mixed[tp], w_out[my_rows])
    send_mixed.wait_recv()
    residual = (residual + dot(mixed[other], w_out[their_rows])).astype(BF16)

    values = residual.astype(F32)
    mine_square = jnp.sum(values * values, axis=1, keepdims=True)
    squares[tp] = jnp.broadcast_to(mine_square, squares.shape[1:])
    send_squares = to_pair(squares.at[tp], squares.at[tp], 3)
    send_squares.start()
    chosen = dot(placing, residual) * expert_gain[:, mine]
    send_squares.wait_recv()
    both = mine_square + squares[other][:, 0:1]
    scaling = as_row(lax.rsqrt(both / (2 * half) + EPSILON))
    slot_scale = jnp.sum(jnp.where(placed, scaling, 0.0), axis=1, keepdims=True)
    chosen = (chosen * slot_scale).reshape(n_ep, pad, half)
    outgoing[...] = chosen[:, :cap].astype(BF16)

    def far(src, dst, to, index):
        return pltpu.make_async_remote_copy(
            src_ref=src,
            dst_ref=dst,
            send_sem=far_send.at[index],
            recv_sem=far_recv.at[index],
            device_id=(to, tp),
            device_id_type=MESH,
        )

    def dispatch(step, carry):
        to = lax.rem(ep + step, n_ep)
        far(outgoing.at[to], recv.at[tp, ep], to, 0).start()
        return carry

    lax.fori_loop(1, n_ep, dispatch, 0)
    recv[tp, ep] = outgoing[ep]
    some = pl.ds(0, n_ep - 1)
    all_dispatched = far(outgoing.at[some], recv.at[tp, some], ep, 0)
    all_dispatched.wait_recv()
    forward = to_pair(recv.at[tp], recv.at[tp], 4)
    forward.start()
    for load in loads[5:]:
        load.wait()
    stage[0, :, :cap] = recv[tp].astype(F32)
    own_rows = stage[0].reshape(slots, half).astype(BF16)
    gate_part = dot(own_rows, w_gate[mine])
    up_part = dot(own_rows, w_up[mine])
    forward.wait_recv()
    stage[1, :, :cap] = recv[other].astype(F32)
    peer_rows = stage[1].reshape(slots, half).astype(BF16)
    gate_part = gate_part + dot(peer_rows, w_gate[theirs])
    up_part = up_part + dot(peer_rows, w_up[theirs])
    hid[tp] = (jax.nn.silu(gate_part) * up_part).astype(BF16)
    send_hid = to_pair(hid.at[tp], hid.at[tp], 5)
    send_hid.start()
    result = dot(hid[tp], w_down[tp])
    send_down.wait_recv()
    send_hid.wait_recv()
    result = result + dot(hid[other], w_down[other])
    ret[...] = result.reshape(n_ep, pad, half)[:, :cap].astype(BF16)

    def give_back(step, carry):
        to = lax.rem(ep + step, n_ep)
        far(ret.at[to], back.at[ep], to, 1).start()
        return carry

    lax.fori_loop(1, n_ep, give_back, 0)
    back[ep] = ret[ep]
    all_returned = far(ret.at[some], back.at[some], ep, 1)
    all_returned.wait_recv()
    back_stage[:, :cap] = back[...].astype(F32)
    rows = back_stage[...].reshape(slots, half).astype(BF16)
    total = weight_a * dot(pick_a, rows) + weight_b * dot(pick_b, rows)
    layer_out[...] = (values + total).astype(BF16)

    for copy in (send_tokens, send_down, send_mixed, send_squares, forward, send_hid):
        copy.wait_send()
    all_dispatched.wait_send()
    all_returned.wait_send()


def local(n_ep, *args):
    names = list(args)
    tokens, conv_state, hidden_state = names[:3]
    seq, half = tokens.shape
    chans = hidden_state.shape[1]
    hidden_units = names[15].shape[2]
    cap = 2 * max(1, seq // n_ep)
    pad = -(-cap // 8) * 8
    for at in (3, 9, 11, 13):
        names[at] = names[at].reshape(1, -1)
    names[1] = conv_state.transpose(1, 0, 2)
    for at in (12, 14):
        names[at] = names[at].T
    vmem = pl.BlockSpec(memory_space=pltpu.VMEM)
    hbm = pl.BlockSpec(memory_space=pltpu.HBM)
    specs = [vmem] * len(names)
    for at in (4, 5, 10, 15, 16, 17):
        specs[at] = hbm
    return pl.pallas_call(
        functools.partial(kernel, n_ep, cap),
        out_shape=(
            pltpu.VMEM((seq, half), BF16),
            pltpu.VMEM((seq, chans), F32),
        ),
        in_specs=specs,
        out_specs=(vmem, vmem),
        scratch_shapes=[
            pltpu.VMEM((2, half, chans), BF16),
            pltpu.VMEM((2, half, chans), BF16),
            pltpu.VMEM((2 * chans, half), BF16),
            pltpu.VMEM((2 * half, hidden_units), BF16),
            pltpu.VMEM((2 * half, hidden_units), BF16),
            pltpu.VMEM((2, hidden_units, half), BF16),
            pltpu.VMEM((seq, half), BF16),
            pltpu.VMEM((2, seq, chans), BF16),
            pltpu.VMEM((2, seq, 128), F32),
            pltpu.VMEM((n_ep, cap, half), BF16),
            pltpu.VMEM((2, n_ep, cap, half), BF16),
            pltpu.VMEM((2, n_ep, pad, half), F32),
            pltpu.VMEM((2, n_ep * pad, hidden_units), BF16),
            pltpu.VMEM((n_ep, cap, half), BF16),
            pltpu.VMEM((n_ep, cap, half), BF16),
            pltpu.VMEM((n_ep, pad, half), F32),
            pltpu.SemaphoreType.DMA((8,)),
            pltpu.SemaphoreType.DMA((6,)),
            pltpu.SemaphoreType.DMA((6,)),
            pltpu.SemaphoreType.DMA((2,)),
            pltpu.SemaphoreType.DMA((2,)),
        ],
        compiler_params=pltpu.CompilerParams(
            collective_id=0, has_side_effects=True, vmem_limit_bytes=VMEM_BYTES - 4 * seq * half
        ),
    )(*names)


def solution(mesh):
    return jax.shard_map(
        functools.partial(local, mesh.shape["ep"]),
        mesh=mesh,
        in_specs=(
            P("ep", "tp"),
            P("ep", None, "tp"),
            P("ep", "tp"),
            P(),
            P(None, "tp"),
            P(None, "tp"),
            P(None, "tp"),
            P("tp", None, None),
            P("tp", None, None),
            P("tp"),
            P(None, "tp"),
            P(),
            P("ep", None),
            P("ep"),
            P("ep", None),
            P("ep", None, "tp"),
            P("ep", None, "tp"),
            P("ep", "tp", None),
        ),
        out_specs=(P("ep", "tp"), P("ep", "tp")),
        check_vma=False,
    )
```

```python
import functools

import jax
import jax.numpy as jnp
from jax import lax
from jax.experimental import pallas as pl
from jax.experimental.pallas import tpu as pltpu
from jax.sharding import PartitionSpec as P

EPSILON = 1e-06
RATE_SCALE = 8.0
VMEM_BYTES = 67_043_328
MESH = pl.DeviceIdType.MESH
F32 = jnp.float32
BF16 = jnp.bfloat16


def iota(shape, dim):
    return lax.broadcasted_iota(jnp.int32, shape, dim)


def dot(a, b):
    return jnp.dot(a, b, preferred_element_type=F32)


def minus_expm1(z):
    series = 1.0
    for term in (7.0, 6.0, 5.0, 4.0, 3.0, 2.0):
        series = 1.0 + z * (1.0 / term) * series
    return jnp.where(z > -0.35, -z * series, 1.0 - jnp.exp(z))


def kernel(
    n_ep,
    cap,
    tokens_in,
    conv_state_in,
    hidden_state_in,
    mixer_gain_in,
    branch_weight,
    gelu_weight,
    conv_kernel_in,
    recur_blocks_in,
    input_blocks_in,
    decay_rate_in,
    output_weight,
    expert_gain_in,
    expert_ids_in,
    group_prob_in,
    expert_logit_in,
    expert_gate,
    expert_up,
    expert_down,
    layer_out,
    new_hidden_ref,
    w_branch,
    w_gelu,
    w_out,
    w_gate,
    w_up,
    w_down,
    tok,
    mixed,
    outgoing,
    recv,
    stage,
    hid,
    ret,
    back,
    back_stage,
    tokens,
    conv_state,
    hidden_state,
    mixer_gain,
    conv_kernel,
    recur_blocks,
    input_blocks,
    decay_rate,
    expert_gain,
    expert_ids,
    group_prob,
    expert_logit,
    load_sem,
    small_sem,
    pair_send,
    pair_recv,
    far_send,
    far_recv,
):
    ep = lax.axis_index("ep")
    tp = lax.axis_index("tp")
    other = 1 - tp
    seq, half = tokens.shape
    chans = hidden_state.shape[1]
    pad = stage.shape[2]
    slots = n_ep * pad

    def partner(step):
        if n_ep & (n_ep - 1):
            return lax.rem(ep + step, n_ep)
        to, weight = 0, 1
        while weight < n_ep:
            bit = ep // weight % 2 + step // weight % 2
            to = to + bit % 2 * weight
            weight *= 2
        return to

    def each_partner(act):
        if n_ep <= 16:
            for step in range(n_ep - 1, 0, -1):
                act(partner(step))
        else:

            def body(index, carry):
                act(partner(n_ep - 1 - index))
                return carry

            lax.fori_loop(0, n_ep - 1, body, 0)

    barrier = pltpu.get_barrier_semaphore()

    def greet(to):
        pl.semaphore_signal(barrier, inc=1, device_id=(to, tp), device_id_type=MESH)

    each_partner(greet)
    pl.semaphore_signal(barrier, inc=1, device_id=(ep, other), device_id_type=MESH)

    small_pairs = (
        (tokens_in, tokens),
        (conv_state_in, conv_state),
        (hidden_state_in, hidden_state),
        (mixer_gain_in, mixer_gain),
        (conv_kernel_in, conv_kernel),
        (recur_blocks_in, recur_blocks),
        (input_blocks_in, input_blocks),
        (decay_rate_in, decay_rate),
        (expert_gain_in, expert_gain),
        (expert_ids_in, expert_ids),
        (group_prob_in, group_prob),
        (expert_logit_in, expert_logit),
    )
    smalls = [
        pltpu.make_async_copy(src, dst, small_sem.at[at])
        for at, (src, dst) in enumerate(small_pairs)
    ]
    for load in smalls:
        load.start()
    mine = pl.ds(pl.multiple_of(tp * half, half), half)
    theirs = pl.ds(pl.multiple_of(other * half, half), half)

    loads = [
        pltpu.make_async_copy(branch_weight.at[mine], w_branch.at[tp], load_sem.at[0]),
        pltpu.make_async_copy(gelu_weight.at[mine], w_gelu.at[tp], load_sem.at[1]),
        pltpu.make_async_copy(branch_weight.at[theirs], w_branch.at[other], load_sem.at[2]),
        pltpu.make_async_copy(gelu_weight.at[theirs], w_gelu.at[other], load_sem.at[3]),
        pltpu.make_async_copy(output_weight, w_out, load_sem.at[4]),
        pltpu.make_async_copy(expert_gate.at[0], w_gate, load_sem.at[5]),
        pltpu.make_async_copy(expert_up.at[0], w_up, load_sem.at[6]),
        pltpu.make_async_copy(expert_down.at[0, :, mine], w_down.at[tp], load_sem.at[7]),
    ]

    def to_pair(src, dst, index):
        return pltpu.make_async_remote_copy(
            src_ref=src,
            dst_ref=dst,
            send_sem=pair_send.at[index],
            recv_sem=pair_recv.at[index],
            device_id=(ep, other),
            device_id_type=MESH,
        )

    stage[...] = jnp.zeros_like(stage)
    back_stage[...] = jnp.zeros_like(back_stage)
    for load in smalls:
        load.wait()
    for load in loads:
        load.start()
    eye = iota((seq, seq), 0) == iota((seq, seq), 1)

    def as_row(column):
        return jnp.sum(jnp.where(eye, column, 0.0), axis=0, keepdims=True)

    def as_column(row):
        return jnp.sum(jnp.where(eye, row, 0.0), axis=1, keepdims=True)

    ids = expert_ids[...].astype(F32)
    first, second = as_column(ids[0:1]), as_column(ids[1:2])
    lane_e = iota((seq, n_ep), 1).astype(F32)
    is_first, is_second = lane_e == first, lane_e == second
    named = jnp.where(is_first | is_second, 1.0, 0.0).astype(BF16)
    before = jnp.where(iota((seq, seq), 1) < iota((seq, seq), 0), 1.0, 0.0).astype(BF16)
    earlier = dot(before, named)

    def slot_of(chosen, hits):
        rank = jnp.sum(jnp.where(hits, earlier, 0.0), axis=1, keepdims=True)
        return chosen * float(pad) + rank

    slot_a, slot_b = slot_of(first, is_first), slot_of(second, is_second)

    lane_s = iota((seq, slots), 1).astype(F32)
    pick_a = jnp.where(lane_s == slot_a, 1.0, 0.0).astype(BF16)
    pick_b = jnp.where(lane_s == slot_b, 1.0, 0.0).astype(BF16)
    row_s = iota((slots, seq), 0).astype(F32)
    placed = (row_s == as_row(slot_a)) | (row_s == as_row(slot_b))
    placing = jnp.where(placed, 1.0, 0.0).astype(BF16)
    logit_exp = jnp.exp(expert_logit[...])
    weights = group_prob[...] * logit_exp / jnp.sum(logit_exp, axis=0, keepdims=True)
    weight_a, weight_b = as_column(weights[0:1]), as_column(weights[1:2])

    taps = conv_kernel[...]
    stored = sum(conv_state[j].astype(F32) * taps[j : j + 1] for j in range(3))

    blocks, block = recur_blocks.shape[0], recur_blocks.shape[1]
    wide = 2 * block
    twice = jnp.where(
        lax.rem(iota((block, wide), 1), block) == iota((block, wide), 0), 1.0, 0.0
    ).astype(BF16)
    on_diagonal = (iota((wide, wide), 0) < block) == (iota((wide, wide), 1) < block)

    def pair_map(ref, index):
        rows = jnp.concatenate([ref[2 * index], ref[2 * index + 1]], axis=0)
        return jnp.where(on_diagonal, dot(rows, twice), 0.0).astype(BF16)

    recur_maps = [pair_map(recur_blocks, i) for i in range(blocks // 2)]
    input_maps = [pair_map(input_blocks, i) for i in range(blocks // 2)]

    own = tokens[...].astype(F32)
    own_scaled = (own * mixer_gain[:, mine]).astype(BF16)
    own_square = jnp.sum(own * own, axis=1, keepdims=True)
    loads[0].wait()
    branch = dot(own_scaled, w_branch[tp])
    loads[1].wait()
    gelu_input = dot(own_scaled, w_gelu[tp])

    pl.semaphore_wait(barrier, n_ep)
    send_tokens = to_pair(tokens, tok, 0)
    send_tokens.start()
    send_down = to_pair(expert_down.at[0, :, theirs], w_down.at[tp], 1)
    send_down.start()

    send_tokens.wait_recv()
    peer = tok[...].astype(F32)
    peer_scaled = (peer * mixer_gain[:, theirs]).astype(BF16)
    total_square = own_square + jnp.sum(peer * peer, axis=1, keepdims=True)
    scale = lax.rsqrt(total_square / (2 * half) + EPSILON)
    loads[2].wait()
    branch = ((branch + dot(peer_scaled, w_branch[other])) * scale).astype(BF16)
    loads[3].wait()
    gelu_input = ((gelu_input + dot(peer_scaled, w_gelu[other])) * scale).astype(BF16)

    convolved = (stored + branch.astype(F32) * taps[3:4]).astype(BF16)
    pieces = [convolved[:, wide * i : wide * (i + 1)] for i in range(blocks // 2)]
    recur_pre = jnp.concatenate([dot(x, m) for x, m in zip(pieces, recur_maps)], axis=1)
    input_pre = jnp.concatenate([dot(x, m) for x, m in zip(pieces, input_maps)], axis=1)
    recur_gate = jax.nn.sigmoid(recur_pre)
    input_gate = jax.nn.sigmoid(input_pre)
    log_decay = -RATE_SCALE * recur_gate * decay_rate[...]
    new_hidden = jnp.exp(log_decay) * hidden_state[...] + jnp.sqrt(
        minus_expm1(2.0 * log_decay)
    ) * (input_gate * convolved.astype(F32))
    mixed[tp] = (new_hidden * jax.nn.gelu(gelu_input.astype(F32), approximate=True)).astype(BF16)
    send_mixed = to_pair(mixed.at[tp], mixed.at[tp], 2)
    send_mixed.start()
    new_hidden_ref[...] = new_hidden
    loads[4].wait()
    my_rows = pl.ds(pl.multiple_of(tp * chans, chans), chans)
    their_rows = pl.ds(pl.multiple_of(other * chans, chans), chans)
    residual = own + dot(mixed[tp], w_out[my_rows])
    send_mixed.wait_recv()
    residual = (residual + dot(mixed[other], w_out[their_rows])).astype(BF16)

    values = residual.astype(F32)
    chosen = dot(placing, residual).reshape(n_ep, pad, half)
    outgoing[...] = chosen[:, :cap].astype(BF16)

    def far(src, dst, to, index):
        return pltpu.make_async_remote_copy(
            src_ref=src,
            dst_ref=dst,
            send_sem=far_send.at[index],
            recv_sem=far_recv.at[index],
            device_id=(to, tp),
            device_id_type=MESH,
        )

    each_partner(lambda to: far(outgoing.at[to], recv.at[tp, ep], to, 0).start())
    recv[tp, ep] = outgoing[ep]
    some = pl.ds(0, n_ep - 1)
    all_dispatched = far(outgoing.at[some], recv.at[tp, some], ep, 0)
    all_dispatched.wait_recv()
    forward = to_pair(recv.at[tp], recv.at[tp], 3)
    forward.start()
    for load in loads[5:]:
        load.wait()
    stage[0, :, :cap] = recv[tp].astype(F32)
    raw = stage[0].reshape(slots, half)
    row_square = jnp.sum(raw * raw, axis=1, keepdims=True)
    own_rows = (raw * expert_gain[:, mine]).astype(BF16)
    gate_part = dot(own_rows, w_gate[mine])
    up_part = dot(own_rows, w_up[mine])
    forward.wait_recv()
    stage[1, :, :cap] = recv[other].astype(F32)
    raw = stage[1].reshape(slots, half)
    row_square = row_square + jnp.sum(raw * raw, axis=1, keepdims=True)
    row_scale = lax.rsqrt(row_square / (2 * half) + EPSILON)
    peer_rows = (raw * expert_gain[:, theirs]).astype(BF16)
    gate_part = (gate_part + dot(peer_rows, w_gate[theirs])) * row_scale
    up_part = (up_part + dot(peer_rows, w_up[theirs])) * row_scale
    hid[tp] = (jax.nn.silu(gate_part) * up_part).astype(BF16)
    send_hid = to_pair(hid.at[tp], hid.at[tp], 4)
    send_hid.start()
    result = dot(hid[tp], w_down[tp])
    send_down.wait_recv()
    send_hid.wait_recv()
    result = result + dot(hid[other], w_down[other])
    ret[...] = result.reshape(n_ep, pad, half)[:, :cap].astype(BF16)

    each_partner(lambda to: far(ret.at[to], back.at[ep], to, 1).start())
    back[ep] = ret[ep]
    all_returned = far(ret.at[some], back.at[some], ep, 1)
    all_returned.wait_recv()
    back_stage[:, :cap] = back[...].astype(F32)
    rows = back_stage[...].reshape(slots, half).astype(BF16)
    total = weight_a * dot(pick_a, rows) + weight_b * dot(pick_b, rows)
    layer_out[...] = (values + total).astype(BF16)

    for copy in (send_tokens, send_down, send_mixed, forward, send_hid):
        copy.wait_send()
    all_dispatched.wait_send()
    all_returned.wait_send()


def write_out(rows, hidden, rows_out, hidden_out, sems):
    copies = [
        pltpu.make_async_copy(rows, rows_out, sems.at[0]),
        pltpu.make_async_copy(hidden, hidden_out, sems.at[1]),
    ]
    for copy in copies:
        copy.start()
    for copy in copies:
        copy.wait()


def local(n_ep, *args):
    names = list(args)
    tokens, conv_state, hidden_state = names[:3]
    seq, half = tokens.shape
    chans = hidden_state.shape[1]
    hidden_units = names[15].shape[2]
    cap = 2 * max(1, seq // n_ep)
    pad = -(-cap // 8) * 8
    for at in (3, 9, 11, 13):
        names[at] = names[at].reshape(1, -1)
    names[1] = conv_state.transpose(1, 0, 2)
    for at in (12, 14):
        names[at] = names[at].T
    vmem = pl.BlockSpec(memory_space=pltpu.VMEM)
    hbm = pl.BlockSpec(memory_space=pltpu.HBM)
    small = (0, 1, 2, 3, 6, 7, 8, 9, 11, 12, 13, 14)
    results = pl.pallas_call(
        functools.partial(kernel, n_ep, cap),
        out_shape=(
            pltpu.VMEM((seq, half), BF16),
            pltpu.VMEM((seq, chans), F32),
        ),
        in_specs=[hbm] * len(names),
        out_specs=(vmem, vmem),
        scratch_shapes=[
            pltpu.VMEM((2, half, chans), BF16),
            pltpu.VMEM((2, half, chans), BF16),
            pltpu.VMEM((2 * chans, half), BF16),
            pltpu.VMEM((2 * half, hidden_units), BF16),
            pltpu.VMEM((2 * half, hidden_units), BF16),
            pltpu.VMEM((2, hidden_units, half), BF16),
            pltpu.VMEM((seq, half), BF16),
            pltpu.VMEM((2, seq, chans), BF16),
            pltpu.VMEM((n_ep, cap, half), BF16),
            pltpu.VMEM((2, n_ep, cap, half), BF16),
            pltpu.VMEM((2, n_ep, pad, half), F32),
            pltpu.VMEM((2, n_ep * pad, hidden_units), BF16),
            pltpu.VMEM((n_ep, cap, half), BF16),
            pltpu.VMEM((n_ep, cap, half), BF16),
            pltpu.VMEM((n_ep, pad, half), F32),
            *[pltpu.VMEM(names[at].shape, names[at].dtype) for at in small],
            pltpu.SemaphoreType.DMA((8,)),
            pltpu.SemaphoreType.DMA((len(small),)),
            pltpu.SemaphoreType.DMA((5,)),
            pltpu.SemaphoreType.DMA((5,)),
            pltpu.SemaphoreType.DMA((2,)),
            pltpu.SemaphoreType.DMA((2,)),
        ],
        compiler_params=pltpu.CompilerParams(
            collective_id=0, has_side_effects=True, vmem_limit_bytes=VMEM_BYTES - 4 * seq * half
        ),
    )(*names)
    return pl.pallas_call(
        write_out,
        out_shape=(
            jax.ShapeDtypeStruct((seq, half), BF16),
            jax.ShapeDtypeStruct((seq, chans), F32),
        ),
        in_specs=[pl.BlockSpec(memory_space=pltpu.VMEM)] * 2,
        out_specs=(hbm, hbm),
        scratch_shapes=[pltpu.SemaphoreType.DMA((2,))],
        compiler_params=pltpu.CompilerParams(vmem_limit_bytes=1 << 20),
    )(*results)


def solution(mesh):
    return jax.shard_map(
        functools.partial(local, mesh.shape["ep"]),
        mesh=mesh,
        in_specs=(
            P("ep", "tp"),
            P("ep", None, "tp"),
            P("ep", "tp"),
            P(),
            P(None, "tp"),
            P(None, "tp"),
            P(None, "tp"),
            P("tp", None, None),
            P("tp", None, None),
            P("tp"),
            P(None, "tp"),
            P(),
            P("ep", None),
            P("ep"),
            P("ep", None),
            P("ep", None, "tp"),
            P("ep", None, "tp"),
            P("ep", "tp", None),
        ),
        out_specs=(P("ep", "tp"), P("ep", "tp")),
        check_vma=False,
    )
```
